32 devices in a mesh: fs: 4 (over z), tp: 4 (over y, x), rep: 2 (over core).
Axes of the slice: x: 2, y: 2, z: 4, core: 2. Of those that a mesh axis runs over, the one named last changes fastest.
Arguments:
- up_weight: float32 [2048, 8192], P('fs', ('tp', 'rep')), may hold values from -0.125 to 0.125
- up_momentum: float32 [2048, 8192], P('fs', ('tp', 'rep')), may hold values from -24 to 24
- up_grads: bfloat16 [2, 2048, 8192], P('rep', 'fs', 'tp'), may hold values from -2.09375 to 2.09375
- out_weight: float32 [2048, 2048], P('fs', ('tp', 'rep')), may hold values from -0.125 to 0.125
- out_momentum: float32 [2048, 2048], P('fs', ('tp', 'rep')), may hold values from -24 to 24
- out_grads: bfloat16 [2, 2048, 2048], P('rep', 'fs', 'tp'), may hold values from -2.09375 to 2.09375
Outputs:
- up_weight_new: float32 [2048, 8192], P('fs', ('tp', 'rep'))
- up_momentum_new: float32 [2048, 8192], P('fs', ('tp', 'rep'))
- up_direction: float32 [2048, 8192], P('fs', ('tp', 'rep'))
- out_weight_new: float32 [2048, 2048], P('fs', ('tp', 'rep'))
- out_momentum_new: float32 [2048, 2048], P('fs', ('tp', 'rep'))
- out_direction: float32 [2048, 2048], P('fs', ('tp', 'rep'))
The draws below stay inside these ranges and needn't reach their ends.
All inputs are finite; a program needn't handle non-finite values.
Results may differ from the reference program's by a relative error of at most 0.039.
Values may be sent and summed in bfloat16 or wider, within the bound.
No kernel may reach another device: no remote copies, remote signals or barrier semaphores. Data moves between devices by JAX's collectives and lax.ppermute only.
A program may use at most 64 MiB of HBM per device.

```python
import math
import jax
import jax.numpy as jnp
from jax import lax

D = 2048
FF = 8192
DMIX = 2048
ITERS = 3
N_REP = 2


def spread_rows(key, row_count, width):
    keys = jax.random.split(key, 4)
    base = jax.random.normal(keys[0], (row_count, width), jnp.float32)
    base = jnp.clip(base, -5.5, 5.5)
    group_rows = row_count // 16
    group_scale = jnp.exp(jax.random.uniform(keys[1], (16,), jnp.float32, math.log(0.12), math.log(3.0)))
    row_scale = jnp.exp(jax.random.uniform(keys[2], (row_count,), jnp.float32, math.log(0.7), math.log(1.4)))
    scale = group_scale[jnp.arange(row_count) // group_rows] * row_scale
    return base * scale[:, None]


def draw_up_momentum(key, part):
    return spread_rows(jax.random.fold_in(key, 11), D, FF)


def draw_out_momentum(key, part):
    return spread_rows(jax.random.fold_in(key, 23), DMIX, D)


def level_of(stream_key, shape, pieces, least, top_value):
    def one(position, parts):
        steps = jax.random.uniform(jax.random.fold_in(jax.random.fold_in(stream_key, 6), position), (parts,), jnp.float32, least / len(pieces), top_value / len(pieces))
        return jnp.repeat(jnp.exp(steps), shape[position] // parts).reshape((-1,) + (1,) * (len(shape) - position - 1))

    loudness = one(*pieces[0])
    for cut in pieces[1:]:
        loudness = loudness * one(*cut)
    return loudness


def scatter_about(rng, extent, deviation, most, shards=(), kind=jnp.bfloat16):
    gain = level_of(rng, extent, shards, -0.22, 0.18) if shards else 1.0
    values = jax.random.normal(rng, extent, jnp.float32) * deviation * gain
    return jnp.minimum(jnp.maximum(values, -most), most).astype(kind)


def setup_inputs(seed: int = 0) -> dict:
    arg_keys = jax.random.split(jax.random.key(seed), 7)
    up_weight = scatter_about(arg_keys[0], (D, FF), D ** -0.5, 0.125, ((0, 4), (1, 8)), jnp.float32)
    up_momentum = draw_up_momentum(jax.random.fold_in(arg_keys[6], 71), 0)
    up_grads = scatter_about(arg_keys[2], (N_REP, D, FF), 0.35, 2.09375, ((0, 2), (1, 4), (2, 4)))
    out_weight = scatter_about(arg_keys[3], (DMIX, D), DMIX ** -0.5, 0.125, ((0, 4), (1, 8)), jnp.float32)
    out_momentum = draw_out_momentum(jax.random.fold_in(arg_keys[6], 71), 0)
    out_grads = scatter_about(arg_keys[5], (N_REP, DMIX, D), 0.35, 2.09375, ((0, 2), (1, 4), (2, 4)))
    return dict(up_weight=up_weight, up_momentum=up_momentum, up_grads=up_grads, out_weight=out_weight, out_momentum=out_momentum, out_grads=out_grads)


MOMENT = 0.9
RATE = 0.02
COEF_A = 3.4445
COEF_B = -4.775
COEF_C = 2.0315

def orthogonal(moment):
    current = moment
    for iteration in range(ITERS):
        values = current.astype(jnp.bfloat16)
        gram = jnp.dot(values, values.T, preferred_element_type=jnp.float32)
        if iteration == 0:
            square = 1.0 / (jnp.sqrt(jnp.sum(gram * gram)) + 1.0)
            factor = jnp.sqrt(square)
        else:
            square = 1.0
            factor = 1.0
        halved = (gram * square).astype(jnp.bfloat16)
        product = factor * jnp.dot(halved, values, preferred_element_type=jnp.float32)
        second = jnp.dot(halved, product.astype(jnp.bfloat16), preferred_element_type=jnp.float32)
        current = COEF_A * factor * current + COEF_B * product + COEF_C * second
    return current

def update(weight, momentum, grads):
    grad = lax.optimization_barrier(jnp.sum(grads.astype(jnp.float32), axis=0))
    moment = MOMENT * momentum + grad
    direction = orthogonal(moment) * math.sqrt(momentum.shape[1])
    return (weight - RATE * direction, moment, direction)

def reference(up_weight, up_momentum, up_grads, out_weight, out_momentum, out_grads):
    up_new, up_moment, up_step = update(up_weight, up_momentum, up_grads)
    out_new, out_moment, out_step = update(out_weight, out_momentum, out_grads)
    return (up_new, up_moment, up_step, out_new, out_moment, out_step)
```

```python
import math

import jax
import jax.numpy as jnp
from jax import lax
from jax.sharding import PartitionSpec as P

ITERS = 3


MOMENT = 0.9
RATE = 0.02
COEF_A = 3.4445
COEF_B = -4.775
COEF_C = 2.0315


def rows_times(rows, matrix):
    return lax.dot_general(
        rows.astype(jnp.bfloat16),
        matrix,
        (((1,), (0,)), ((), ())),
        preferred_element_type=jnp.float32,
    )


def local_gram(values, columns):
    return lax.dot_general(
        values, columns, (((1,), (1,)), ((), ())), preferred_element_type=jnp.float32
    )


def reduce_grads(grads):
    return lax.psum_scatter(grads[0], "rep", scatter_dimension=1, tiled=True).astype(jnp.float32)


def on_device(up_weight, up_momentum, up_grads, out_weight, out_momentum, out_grads):
    n_rep, n_tp = lax.axis_size("rep"), lax.axis_size("tp")
    group = n_tp * n_rep
    moments = [
        MOMENT * up_momentum + reduce_grads(up_grads),
        MOMENT * out_momentum + reduce_grads(out_grads),
    ]
    values = [entry.astype(jnp.bfloat16) for entry in moments]
    columns = [lax.all_gather(entry, "fs", axis=0, tiled=True) for entry in values]
    partial = jnp.concatenate(
        [local_gram(values[k], columns[k]).astype(jnp.bfloat16) for k in range(2)], axis=0
    )
    mine = lax.psum_scatter(partial, ("rep", "tp"), scatter_dimension=0, tiled=True)
    block = mine.shape[0]
    shard = values[0].shape[0]
    size = mine.shape[1]
    half = n_rep // 2
    rep = lax.axis_index("rep")
    if half == 1:
        gram = lax.all_gather(mine, ("fs", "tp"), axis=0, tiled=True)
    else:
        both = lax.all_gather(mine, ("fs", "rep", "tp"), axis=0, tiled=True)
        both = both.reshape(-1, 2, shard, size)
        gram = lax.dynamic_index_in_dim(both, rep // half, 1, keepdims=False).reshape(size, size)
    first = lax.axis_index("fs") * shard + ((rep % half) * n_tp + lax.axis_index("tp")) * block
    wide = gram.astype(jnp.float32)
    square = 1.0 / (jnp.sqrt(jnp.sum(wide * wide)) + 1.0)
    factor = jnp.sqrt(square)

    step0 = (
        COEF_B * square * wide + (COEF_C * square * square) * rows_times(gram, gram)
    ).astype(jnp.bfloat16)
    turned = ((COEF_A * square) * wide + square * rows_times(step0, gram)).astype(jnp.bfloat16)
    gram1 = (COEF_A * turned.astype(jnp.float32) + rows_times(turned, step0)).astype(jnp.bfloat16)

    def apply1(rows):
        once = rows_times(rows, gram1)
        return COEF_A * rows + COEF_B * once + COEF_C * rows_times(once, gram1)

    step0_rows = lax.dynamic_slice_in_dim(step0, first, block, 0).astype(jnp.float32)
    gram1_rows = lax.dynamic_slice_in_dim(gram1, first, block, 0).astype(jnp.float32)
    step1_rows = COEF_B * gram1_rows + COEF_C * rows_times(gram1_rows, gram1)
    gram2_rows = apply1(COEF_A * gram1_rows + rows_times(step1_rows, gram1))
    gram2_square = apply1(rows_times(apply1(gram2_rows), gram1))
    step2_rows = COEF_B * gram2_rows + COEF_C * gram2_square
    joined = COEF_A * step1_rows + apply1(step2_rows)
    total = COEF_A * COEF_A * step0_rows + COEF_A * joined + rows_times(joined, step0)
    row_ids = first + lax.broadcasted_iota(jnp.int32, total.shape, 0)
    column_ids = lax.broadcasted_iota(jnp.int32, total.shape, 1)
    total = factor * (total + jnp.where(row_ids == column_ids, COEF_A**ITERS, 0.0))
    maps = lax.all_gather(total.astype(jnp.bfloat16), ("rep", "tp"), axis=0, tiled=True)

    widths = [up_weight.shape[1] * group, out_weight.shape[1] * group]
    directions = [
        math.sqrt(widths[k]) * rows_times(maps[k * shard : (k + 1) * shard], columns[k])
        for k in range(2)
    ]
    return (
        up_weight - RATE * directions[0],
        moments[0],
        directions[0],
        out_weight - RATE * directions[1],
        moments[1],
        directions[1],
    )


def solution(mesh):
    return jax.shard_map(
        on_device,
        mesh=mesh,
        in_specs=(
            P("fs", ("tp", "rep")),
            P("fs", ("tp", "rep")),
            P("rep", "fs", "tp"),
            P("fs", ("tp", "rep")),
            P("fs", ("tp", "rep")),
            P("rep", "fs", "tp"),
        ),
        out_specs=(
            P("fs", ("tp", "rep")),
            P("fs", ("tp", "rep")),
            P("fs", ("tp", "rep")),
            P("fs", ("tp", "rep")),
            P("fs", ("tp", "rep")),
            P("fs", ("tp", "rep")),
        ),
        check_vma=False,
    )
```
